32 devices in a mesh: ep: 8 (over z, core), tp: 4 (over y, x).
Axes of the slice: x: 2, y: 2, z: 4, core: 2. Of those that a mesh axis runs over, the one named last changes fastest.
Arguments:
- tokens: bfloat16 [512, 2048], P('ep', 'tp'), may hold values from -6 to 6
- gain_mix: float32 [2048], replicated, may hold values from 0.1 to 1.9
- w_in: bfloat16 [2048, 1024], P(None, 'tp'), may hold values from -0.125 to 0.125
- decay_rate: float32 [64, 64], P('tp'), may hold values from 0.05 to 3
- frequency: float32 [64, 64], P('tp'), may hold values from -3 to 3
- log_step: float32 [64], P('tp'), may hold values from -3 to 0
- input_real: float32 [64, 64, 16], P('tp'), may hold values from -1 to 1
- input_imag: float32 [64, 64, 16], P('tp'), may hold values from -1 to 1
- readout_real: float32 [64, 16, 64], P('tp'), may hold values from -0.75 to 0.75
- readout_imaginary: float32 [64, 16, 64], P('tp'), may hold values from -0.75 to 0.75
- passthrough_scale: float32 [1024], P('tp'), may hold values from -4 to 4
- state_real: float32 [512, 64, 64], P('ep', 'tp'), may hold values from -4 to 4
- state_imag: float32 [512, 64, 64], P('ep', 'tp'), may hold values from -4 to 4
- w_out: bfloat16 [1024, 2048], replicated, may hold values from -0.1875 to 0.1875
- gain_ffn: float32 [2048], replicated, may hold values from 0.1 to 1.9
- expert_choice: int32 [512, 2], P('ep'), may hold values from 0 to 7, all different within a row; in each aligned block of 64 rows (0 to 63, 64 to 127, ...) at most 32 rows name the same one
- expert_weight: float32 [512, 2], P('ep'), may hold values from 0.2 to 1
- w_gate: bfloat16 [8, 2048, 8192], P('ep', None, 'tp'), may hold values from -0.125 to 0.125
- w_up: bfloat16 [8, 2048, 8192], P('ep', None, 'tp'), may hold values from -0.125 to 0.125
- w_down: bfloat16 [8, 8192, 2048], P('ep', 'tp'), may hold values from -0.0625 to 0.0625
Outputs:
- layer_out: bfloat16 [512, 2048], P('ep', 'tp')
- next_state_real: float32 [512, 64, 64], P('ep', 'tp')
- next_state_imaginary: float32 [512, 64, 64], P('ep', 'tp')
The draws below stay inside these ranges and needn't reach their ends.
Inputs may be any that keep to these rules, and one draw needn't show every extreme that they name: `expert_choice`: each row names 2 different experts; in the rows of one index of ep (aligned blocks of 64 rows) no expert is named more than 32 times, a bound that some block reaches.
All inputs are finite; a program needn't handle non-finite values.
Results may differ from the reference program's by a relative error of at most 0.017.
Values may be sent and summed in bfloat16 or wider, within the bound.
A program may use at most 64 MiB of HBM per device.

```python
import math
import jax
import jax.numpy as jnp
import numpy as np
from jax import lax

D = 2048
SSM_WIDTH = 1024
CHANNELS = 16
STATE = 64
FF = 8192
TOP = 2
SEQS = 64
GROUPS = 64
EXPERTS = 8
CAP = 32
ROWS = 512
N_EP = 8
N_TP = 4


def level_of(own_key, shape, shards, low, high):
    def one(position, shards_of):
        heights = jax.random.uniform(jax.random.fold_in(jax.random.fold_in(own_key, 6), position), (shards_of,), jnp.float32, low / len(shards), high / len(shards))
        return jnp.repeat(jnp.exp(heights), shape[position] // shards_of).reshape((-1,) + (1,) * (len(shape) - position - 1))

    level = one(*shards[0])
    for cut in shards[1:]:
        level = level * one(*cut)
    return level


def shared_out(stream_key, own, number, rows, number_of, top, reach, slope):
    ranking = jax.random.permutation(stream_key, number_of)
    heavy_load, common = shares(number_of, rows * top, reach, slope, True), shares(number_of, rows * top, reach, slope, False)
    places = jnp.arange(number_of)

    def named(tallies, offset_by):
        used = int((tallies > 0).sum())
        fixed = max(1, used // 4)
        passed = fixed + (places - fixed + offset_by * (used - fixed)) % max(1, number_of - fixed)
        return jnp.zeros((number_of,), jnp.int32).at[ranking[jnp.where(places < fixed, places, passed)]].set(jnp.asarray(tallies, jnp.int32))

    tallies = jnp.where(number % 4 == 0, named(heavy_load, number // 4), named(common, number - number // 4 - 1))
    mixed = jax.random.permutation(jax.random.fold_in(own, 3), number_of)
    donor, receiver = mixed[0:number_of // 2 * 2:2], mixed[1:number_of // 2 * 2:2]
    slack = jnp.minimum(tallies[donor] - 1, reach - tallies[receiver]) // 2
    slack = jnp.where((donor == ranking[0]) | (receiver == ranking[0]) | (tallies[receiver] == 0), 0, jnp.maximum(slack, 0))
    passed = jax.random.randint(jax.random.fold_in(own, 4), (number_of // 2,), 0, 1 << 20) % (slack + 1)
    tallies = tallies.at[donor].add(-passed).at[receiver].add(passed)
    members = jnp.searchsorted(jnp.cumsum(tallies), jnp.arange(rows * top), side="right").astype(jnp.int32)
    listing = members.reshape(top, rows).T
    listing = listing[jax.random.permutation(jax.random.fold_in(own, 1), rows)]
    offset_by = jax.random.randint(jax.random.fold_in(own, 2), (rows, 1), 0, top)
    return jnp.take_along_axis(listing, (jnp.arange(top)[None, :] + offset_by) % top, axis=1)


def shares(number_of, total, most, slope, full):
    weights = [(1 << 20) // math.isqrt(standing ** slope) + 1 for standing in range(1, number_of + 1)]
    largest = most if full else min(most, max(-(-total // number_of), total * weights[0] // sum(weights)))
    least = 1 if total - largest >= number_of - 1 else 0
    given, spare = [largest] + [least] * (number_of - 1), total - largest - least * (number_of - 1)
    while spare > 0:
        candidates = [i for i in range(1, number_of) if given[i] < largest] or [i for i in range(1, number_of) if given[i] < most]
        mass, budget = sum([weights[i] for i in candidates]), spare
        for i in candidates:
            more = min(most - given[i], max(1, budget * weights[i] // mass), spare)
            given[i] = given[i] + more
            spare = spare - more
    return np.array(given)


def normal_values(rng, shape, deviation, bound, split=(), kind=jnp.bfloat16):
    level = level_of(rng, shape, split, -0.22, 0.18) if split else 1.0
    array = jax.random.normal(rng, shape, jnp.float32) * deviation * level
    return jnp.minimum(jnp.maximum(array, -bound), bound).astype(kind)


def setup_inputs(seed: int = 0) -> dict:
    streams_of = jax.random.split(jax.random.key(seed), 21)
    tokens = normal_values(streams_of[0], (ROWS, D), 1.0, 6.0, ((0, 8), (1, 4)))
    gain_mix = jnp.clip(1.0 + 0.18 * jax.random.normal(streams_of[1], (D,), jnp.float32), 0.1, 1.9)
    w_in = normal_values(streams_of[2], (D, SSM_WIDTH), D ** -0.5, 0.125, ((1, 4),))
    decay_rate = jnp.clip(jnp.exp(math.log(3.0) - 4.0943445 * jax.random.uniform(streams_of[3], (GROUPS, STATE), jnp.float32) ** level_of(streams_of[3], (GROUPS, STATE), ((0, 4),), -0.2, 0.2)), 0.05, 3.0)
    frequency = jnp.clip(jax.random.uniform(streams_of[4], (GROUPS, STATE), jnp.float32, -3.0, 3.0) * level_of(streams_of[4], (GROUPS, STATE), ((0, 4),), -0.4, 0.0), -3.0, 3.0)
    log_step = jnp.clip(-3.0 + 3.0 * jax.random.uniform(streams_of[5], (GROUPS,), jnp.float32) ** level_of(streams_of[5], (GROUPS,), ((0, 4),), -0.2, 0.2), -3.0, 0.0)
    input_real = normal_values(streams_of[6], (GROUPS, STATE, CHANNELS), (2 * CHANNELS) ** -0.5, 1.0, ((0, 4),), jnp.float32)
    input_imag = normal_values(streams_of[7], (GROUPS, STATE, CHANNELS), (2 * CHANNELS) ** -0.5, 1.0, ((0, 4),), jnp.float32)
    readout_real = normal_values(streams_of[8], (GROUPS, CHANNELS, STATE), STATE ** -0.5, 0.75, ((0, 4),), jnp.float32)
    readout_imaginary = normal_values(streams_of[9], (GROUPS, CHANNELS, STATE), STATE ** -0.5, 0.75, ((0, 4),), jnp.float32)
    passthrough_scale = normal_values(streams_of[10], (SSM_WIDTH,), 1.0, 4.0, ((0, 4),), jnp.float32)
    state_real = normal_values(streams_of[11], (ROWS, GROUPS, STATE), 0.5, 4.0, ((0, 8), (1, 4)), jnp.float32)
    state_imag = normal_values(streams_of[12], (ROWS, GROUPS, STATE), 0.5, 4.0, ((0, 8), (1, 4)), jnp.float32)
    w_out = normal_values(streams_of[13], (SSM_WIDTH, D), SSM_WIDTH ** -0.5, 0.1875)
    gain_ffn = jnp.clip(1.0 + 0.18 * jax.random.normal(streams_of[14], (D,), jnp.float32), 0.1, 1.9)
    expert_choice_keys = jax.random.split(jax.random.fold_in(streams_of[15], 1), ROWS // SEQS)
    expert_choice_turns = jax.random.permutation(jax.random.fold_in(streams_of[15], 3), ROWS // SEQS)
    expert_choice = jax.vmap(lambda own, number: shared_out(jax.random.fold_in(streams_of[15], 2), own, number, SEQS, EXPERTS, TOP, CAP, 2))(expert_choice_keys, expert_choice_turns).reshape((ROWS, TOP))
    expert_weight = jnp.clip(0.2 + 0.8 * jax.random.uniform(streams_of[16], (ROWS, TOP), jnp.float32) ** level_of(streams_of[16], (ROWS, TOP), ((0, 8),), -0.2, 0.2), 0.2, 1.0)
    w_gate = normal_values(streams_of[17], (EXPERTS, D, FF), D ** -0.5, 0.125, ((0, 8), (2, 4)))
    w_up = normal_values(streams_of[18], (EXPERTS, D, FF), D ** -0.5, 0.125, ((0, 8), (2, 4)))
    w_down = normal_values(streams_of[19], (EXPERTS, FF, D), FF ** -0.5, 0.0625, ((0, 8), (1, 4)))
    return dict(tokens=tokens, gain_mix=gain_mix, w_in=w_in, decay_rate=decay_rate, frequency=frequency, log_step=log_step, input_real=input_real, input_imag=input_imag, readout_real=readout_real, readout_imaginary=readout_imaginary, passthrough_scale=passthrough_scale, state_real=state_real, state_imag=state_imag, w_out=w_out, gain_ffn=gain_ffn, expert_choice=expert_choice, expert_weight=expert_weight, w_gate=w_gate, w_up=w_up, w_down=w_down)


def rms_norm(values, gains):
    float_values = values.astype(jnp.float32)
    scale = lax.rsqrt(lax.optimization_barrier(jnp.mean(float_values * float_values, axis=-1, keepdims=True)) + 1e-06)
    return (float_values * scale * gains).astype(jnp.bfloat16)

def state_step(drive, real_state, imag_state, decay_rate, frequency, log_step, input_real, input_imag, readout_real, readout_imaginary, passthrough_scale):
    highest_precision = lax.Precision.HIGHEST
    count_of_groups, count_of_channels = (input_real.shape[0], input_real.shape[2])
    step = jnp.exp(log_step)[:, None]
    lam_real = -decay_rate
    magnitude = jnp.exp(lam_real * step)
    abar_real = magnitude * jnp.cos(frequency * step)
    abar_imag = magnitude * jnp.sin(frequency * step)
    denom = lam_real * lam_real + frequency * frequency
    numer = abar_real - 1.0
    factor_real = (numer * lam_real + abar_imag * frequency) / denom
    factor_imag = (abar_imag * lam_real - numer * frequency) / denom
    bbar_real = factor_real[..., None] * input_real - factor_imag[..., None] * input_imag
    bbar_imag = factor_real[..., None] * input_imag + factor_imag[..., None] * input_real
    float_values = drive.astype(jnp.float32).reshape(drive.shape[0], count_of_groups, count_of_channels)
    push_real = jnp.einsum('sgc,gpc->sgp', float_values, bbar_real, precision=highest_precision)
    push_imag = jnp.einsum('sgc,gpc->sgp', float_values, bbar_imag, precision=highest_precision)
    next_state_real = abar_real * real_state - abar_imag * imag_state + push_real
    next_state_imaginary = abar_real * imag_state + abar_imag * real_state + push_imag
    readout_matrix = jnp.einsum('jdr,dyr->jdy', next_state_real, readout_real, precision=highest_precision) - jnp.einsum('jdr,dyr->jdy', next_state_imaginary, readout_imaginary, precision=highest_precision) + passthrough_scale.reshape(count_of_groups, count_of_channels) * float_values
    mixer = jax.nn.gelu(readout_matrix.reshape(drive.shape[0], count_of_groups * count_of_channels)).astype(jnp.bfloat16)
    return (mixer, next_state_real, next_state_imaginary)

def slot_table(routes, expert_count, capacity):
    flat = routes.reshape(-1)
    onehot = (flat[:, None] == jnp.arange(expert_count, dtype=jnp.int32)[None, :]).astype(jnp.int32)
    before = jnp.cumsum(onehot, axis=0) - onehot
    slot = lax.optimization_barrier(jnp.sum(before * onehot, axis=1))
    target = flat * capacity + slot
    return (target[None, :] == jnp.arange(expert_count * capacity, dtype=jnp.int32)[:, None]).astype(jnp.bfloat16)

def reference(tokens, gain_mix, w_in, decay_rate, frequency, log_step, input_real, input_imag, readout_real, readout_imaginary, passthrough_scale, state_real, state_imag, w_out, gain_ffn, expert_choice, expert_weight, w_gate, w_up, w_down):
    normed = rms_norm(tokens, gain_mix)
    drive = jnp.dot(normed, w_in, preferred_element_type=jnp.float32).astype(jnp.bfloat16)
    mixer, next_state_real, next_state_imaginary = state_step(drive, state_real, state_imag, decay_rate, frequency, log_step, input_real, input_imag, readout_real, readout_imaginary, passthrough_scale)
    mixed = jnp.dot(mixer, w_out, preferred_element_type=jnp.float32).astype(jnp.bfloat16)
    after_mix = (tokens.astype(jnp.float32) + mixed.astype(jnp.float32)).astype(jnp.bfloat16)
    normed_ffn = rms_norm(after_mix, gain_ffn)
    group_rows = normed_ffn.reshape(N_EP, SEQS, D)
    routes = expert_choice.reshape(N_EP, SEQS, TOP)
    tables = jax.vmap(lambda block: slot_table(block, EXPERTS, CAP))(routes).astype(jnp.float32)
    repeated = jnp.repeat(group_rows, TOP, axis=1).astype(jnp.float32)
    sent = jnp.einsum('gks,gsd->gkd', tables, repeated).astype(jnp.bfloat16)
    sent = jnp.moveaxis(sent.reshape(N_EP, EXPERTS, CAP, D), 1, 0)
    slice_width = FF // N_TP

    def expert(inputs):
        arrived, gate_w, up_w, down_w = inputs
        flat = arrived.reshape(N_EP * CAP, D)
        gate = jnp.dot(flat, gate_w, preferred_element_type=jnp.float32)
        upper = jnp.dot(flat, up_w, preferred_element_type=jnp.float32)
        hidden = (jax.nn.silu(gate) * upper).astype(jnp.bfloat16)
        pieces = hidden.reshape(N_EP * CAP, N_TP, slice_width).astype(jnp.float32)
        downs = down_w.reshape(N_TP, slice_width, D).astype(jnp.float32)
        partial_value = jnp.einsum('rtf,tfd->rtd', pieces, downs).astype(jnp.bfloat16)
        partial_value = lax.optimization_barrier(partial_value)
        return lax.optimization_barrier(jnp.sum(partial_value.astype(jnp.float32), axis=1)).astype(jnp.bfloat16)
    results = lax.map(expert, (sent, w_gate, w_up, w_down))
    results = jnp.moveaxis(results.reshape(EXPERTS, N_EP, CAP, D), 1, 0).reshape(N_EP, EXPERTS * CAP, D)
    picked = jnp.einsum('gks,gkd->gsd', tables, results.astype(jnp.float32)).reshape(N_EP, SEQS, TOP, D)
    weighted = lax.optimization_barrier(jnp.sum(picked * expert_weight.reshape(N_EP, SEQS, TOP)[..., None], axis=2)).reshape(ROWS, D)
    layer_out = (after_mix.astype(jnp.float32) + weighted).astype(jnp.bfloat16)
    return (layer_out, next_state_real, next_state_imaginary)
```

```python
import functools

import jax
import jax.numpy as jnp
from jax import lax
from jax.experimental import pallas as pl
from jax.experimental.pallas import tpu as pltpu
from jax.sharding import PartitionSpec as P


def state_step(
    drive,
    real_state,
    imag_state,
    decay_rate,
    frequency,
    log_step,
    input_real,
    input_imag,
    readout_real,
    readout_imaginary,
    passthrough_scale,
):
    highest_precision = lax.Precision.HIGHEST
    count_of_groups, count_of_channels = (input_real.shape[0], input_real.shape[2])
    step = jnp.exp(log_step)[:, None]
    lam_real = -decay_rate
    magnitude = jnp.exp(lam_real * step)
    abar_real = magnitude * jnp.cos(frequency * step)
    abar_imag = magnitude * jnp.sin(frequency * step)
    denom = lam_real * lam_real + frequency * frequency
    numer = abar_real - 1.0
    factor_real = (numer * lam_real + abar_imag * frequency) / denom
    factor_imag = (abar_imag * lam_real - numer * frequency) / denom
    bbar_real = factor_real[..., None] * input_real - factor_imag[..., None] * input_imag
    bbar_imag = factor_real[..., None] * input_imag + factor_imag[..., None] * input_real
    float_values = drive.astype(jnp.float32).reshape(
        drive.shape[0], count_of_groups, count_of_channels
    )
    push_real = jnp.einsum("sgc,gpc->sgp", float_values, bbar_real, precision=highest_precision)
    push_imag = jnp.einsum("sgc,gpc->sgp", float_values, bbar_imag, precision=highest_precision)
    next_state_real = abar_real * real_state - abar_imag * imag_state + push_real
    next_state_imaginary = abar_real * imag_state + abar_imag * real_state + push_imag
    readout_matrix = (
        jnp.einsum("jdr,dyr->jdy", next_state_real, readout_real, precision=highest_precision)
        - jnp.einsum(
            "jdr,dyr->jdy", next_state_imaginary, readout_imaginary, precision=highest_precision
        )
        + passthrough_scale.reshape(count_of_groups, count_of_channels) * float_values
    )
    mixer = jax.nn.gelu(
        readout_matrix.reshape(drive.shape[0], count_of_groups * count_of_channels)
    ).astype(jnp.bfloat16)
    return (mixer, next_state_real, next_state_imaginary)


def slot_table(routes, expert_count, capacity):
    flat = routes.reshape(-1)
    onehot = (flat[:, None] == jnp.arange(expert_count, dtype=jnp.int32)[None, :]).astype(jnp.int32)
    before = jnp.cumsum(onehot, axis=0) - onehot
    slot = jnp.sum(before * onehot, axis=1)
    target = flat * capacity + slot
    return (
        target[None, :] == jnp.arange(expert_count * capacity, dtype=jnp.int32)[:, None]
    ).astype(jnp.bfloat16)


def flipped(index, mask, count):
    other = 0
    bit = 1
    while bit < count:
        digit = lax.rem(lax.div(index, bit), 2)
        other = other + bit * ((1 - digit) if mask & bit else digit)
        bit *= 2
    return other


def expert_kernel(
    ep_count,
    tp_count,
    normed_ref,
    after_ref,
    table_ref,
    high_ref,
    low_ref,
    gate_hbm,
    up_hbm,
    down_hbm,
    out_ref,
    gate_w,
    up_w,
    down_w,
    outgoing,
    arrived,
    gate_sum,
    up_sum,
    hidden,
    parts,
    parts_in,
    results,
    returned,
    weight_sem,
    out_send,
    out_recv,
    near_send,
    near_recv,
    far_send,
    far_recv,
    part_send,
    part_recv,
    back_send,
    back_recv,
):
    me_ep, me_tp = lax.axis_index("ep"), lax.axis_index("tp")
    capacity, width = outgoing.shape[1], outgoing.shape[2]
    half = ep_count // 2
    peers = sorted(range(1, tp_count), key=lambda p: (bin(p).count("1"), p))
    near = [p for p in peers if bin(p).count("1") == 1]
    far = [p for p in peers if p not in near]
    tp_of = {p: flipped(me_tp, p, tp_count) for p in range(tp_count)}
    ep_of = {j: flipped(me_ep, j, ep_count) for j in range(ep_count)}

    def remote(src, dst, send, recv, **where):
        return pltpu.make_async_remote_copy(
            src_ref=src,
            dst_ref=dst,
            send_sem=send,
            recv_sem=recv,
            device_id=where,
            device_id_type=pl.DeviceIdType.MESH,
        )

    order = [0] + peers
    loads = {}
    for p in order:
        rows = pl.ds(pl.multiple_of(tp_of[p] * width, width), width)
        loads[0, p] = pltpu.make_async_copy(gate_hbm.at[0, rows], gate_w.at[p], weight_sem.at[0, p])
        loads[1, p] = pltpu.make_async_copy(up_hbm.at[0, rows], up_w.at[p], weight_sem.at[1, p])
        loads[0, p].start()
        loads[1, p].start()
    down_order = far + near + [0]
    for p in down_order:
        columns = pl.ds(pl.multiple_of(tp_of[p] * width, width), width)
        loads[2, p] = pltpu.make_async_copy(
            down_hbm.at[0, :, columns], down_w.at[p], weight_sem.at[2, p]
        )
        loads[2, p].start()

    barrier = pltpu.get_barrier_semaphore()
    for p in peers:
        pl.semaphore_signal(
            barrier, inc=1, device_id={"tp": tp_of[p]}, device_id_type=pl.DeviceIdType.MESH
        )
    for j in range(1, ep_count):
        pl.semaphore_signal(
            barrier, inc=1, device_id={"ep": ep_of[j]}, device_id_type=pl.DeviceIdType.MESH
        )
    sent = jnp.dot(table_ref[...], normed_ref[...], preferred_element_type=jnp.float32)
    outgoing[...] = sent.astype(jnp.bfloat16).reshape(outgoing.shape)
    arrived[0, 0] = outgoing[me_ep]
    pl.semaphore_wait(barrier, len(peers) + ep_count - 1)

    out_copies = {}
    for j in range(1, ep_count):
        out_copies[j] = remote(
            outgoing.at[ep_of[j]], arrived.at[0, j], out_send.at[j], out_recv.at[j], ep=ep_of[j]
        )
        out_copies[j].start()
    near_copies, far_copies = {}, {}
    for part in range(2):
        for j in range(part * half, part * half + half):
            if j:
                out_copies[j].wait_recv()
            for p in near:
                near_copies[p, j] = remote(
                    arrived.at[0, j],
                    arrived.at[p, j],
                    near_send.at[p, j],
                    near_recv.at[p, j],
                    tp=tp_of[p],
                )
                near_copies[p, j].start()
        for p in far:
            blocks = pl.ds(part * half, half)
            far_copies[p, part] = remote(
                arrived.at[0, blocks],
                arrived.at[p, blocks],
                far_send.at[p, part],
                far_recv.at[p, part],
                tp=tp_of[p],
            )
            far_copies[p, part].start()

    rows = ep_count * capacity
    hidden_width = hidden.shape[1]
    tile = next(t for t in (512, 256, 128) if hidden_width % t == 0)
    for place, p in enumerate(order):
        if p in near:
            for j in range(ep_count):
                near_copies[p, j].wait_recv()
        elif p:
            for part in range(2):
                far_copies[p, part].wait_recv()
        loads[0, p].wait()
        loads[1, p].wait()

        @pl.loop(0, hidden_width // tile)
        def _(n, place=place, p=p):
            columns = pl.ds(pl.multiple_of(n * tile, tile), tile)
            block = arrived[p].reshape(rows, width)
            gate = jnp.dot(block, gate_w[p, :, columns], preferred_element_type=jnp.float32)
            upper = jnp.dot(block, up_w[p, :, columns], preferred_element_type=jnp.float32)
            if place:
                gate = gate + gate_sum[:, columns]
                upper = upper + up_sum[:, columns]
            if place == len(order) - 1:
                hidden[:, columns] = (jax.nn.silu(gate) * upper).astype(jnp.bfloat16)
            else:
                gate_sum[:, columns] = gate
                up_sum[:, columns] = upper

    def part_copy(p, part):
        blocks = pl.ds((1 - part) * half * capacity, half * capacity)
        return remote(
            parts.at[p, blocks],
            parts_in.at[p, blocks],
            part_send.at[p, part],
            part_recv.at[p, part],
            tp=tp_of[p],
        )

    part_copies = {(p, part): part_copy(p, part) for p in peers for part in range(2)}
    cut = next(t for t in (256, 128) if width % t == 0)
    for p in down_order:
        loads[2, p].wait()

        @pl.loop(0, width // cut)
        def _(n, p=p):
            columns = pl.ds(pl.multiple_of(n * cut, cut), cut)
            parts[p, :, columns] = jnp.dot(
                hidden[...], down_w[p, :, columns], preferred_element_type=jnp.float32
            ).astype(jnp.bfloat16)

        if p:
            part_copies[p, 0].start()
        if p == down_order[-2]:
            for q in down_order[:-1]:
                part_copies[q, 1].start()

    back_copies = {}
    for part in range(2):
        blocks = pl.ds((1 - part) * half * capacity, half * capacity)
        total = None
        for p in range(tp_count):
            if p:
                part_copies[p, part].wait_recv()
                piece = parts_in[p, blocks].astype(jnp.float32)
            else:
                piece = parts[0, blocks].astype(jnp.float32)
            total = piece if total is None else total + piece
        first = (1 - part) * half
        results[pl.ds(first, half)] = total.astype(jnp.bfloat16).reshape(half, capacity, width)
        for j in reversed(range(first, first + half)):
            if j:
                back_copies[j] = remote(
                    results.at[j],
                    returned.at[me_ep],
                    back_send.at[j],
                    back_recv.at[j],
                    ep=ep_of[j],
                )
                back_copies[j].start()
    returned[me_ep] = results[0]
    for j in range(1, ep_count):
        remote(
            results.at[j], returned.at[ep_of[j]], back_send.at[j], back_recv.at[j], ep=ep_of[j]
        ).wait_recv()
    everything = returned[...].reshape(rows, width)
    weighted = jnp.dot(high_ref[...], everything, preferred_element_type=jnp.float32)
    weighted = weighted + jnp.dot(low_ref[...], everything, preferred_element_type=jnp.float32)
    out_ref[...] = (after_ref[...].astype(jnp.float32) + weighted).astype(jnp.bfloat16)
    for copies in (out_copies, near_copies, far_copies, part_copies, back_copies):
        for copy in copies.values():
            copy.wait_send()


def expert_call(normed, after, table, high, low, w_gate, w_up, w_down, ep_count, tp_count):
    row_count, width = normed.shape
    capacity = table.shape[0] // ep_count
    slots = ep_count * capacity
    hidden_width = w_gate.shape[2]
    bf16, f32 = jnp.bfloat16, jnp.float32
    dma = pltpu.SemaphoreType.DMA
    vmem = pl.BlockSpec(memory_space=pltpu.VMEM)
    hbm = pl.BlockSpec(memory_space=pl.ANY)
    return pl.pallas_call(
        functools.partial(expert_kernel, ep_count, tp_count),
        out_shape=jax.ShapeDtypeStruct((row_count, width), bf16),
        in_specs=[vmem] * 5 + [hbm] * 3,
        out_specs=vmem,
        scratch_shapes=[
            pltpu.VMEM((tp_count, width, hidden_width), bf16),
            pltpu.VMEM((tp_count, width, hidden_width), bf16),
            pltpu.VMEM((tp_count, hidden_width, width), bf16),
            pltpu.VMEM((ep_count, capacity, width), bf16),
            pltpu.VMEM((tp_count, ep_count, capacity, width), bf16),
            pltpu.VMEM((slots, hidden_width), f32),
            pltpu.VMEM((slots, hidden_width), f32),
            pltpu.VMEM((slots, hidden_width), bf16),
            pltpu.VMEM((tp_count, slots, width), bf16),
            pltpu.VMEM((tp_count, slots, width), bf16),
            pltpu.VMEM((ep_count, capacity, width), bf16),
            pltpu.VMEM((ep_count, capacity, width), bf16),
            dma((3, tp_count)),
            dma((ep_count,)),
            dma((ep_count,)),
            dma((tp_count, ep_count)),
            dma((tp_count, ep_count)),
            dma((tp_count, 2)),
            dma((tp_count, 2)),
            dma((tp_count, 2)),
            dma((tp_count, 2)),
            dma((ep_count,)),
            dma((ep_count,)),
        ],
        compiler_params=pltpu.CompilerParams(
            collective_id=0, has_side_effects=True, vmem_limit_bytes=60 * 1024 * 1024
        ),
    )(normed, after, table, high, low, w_gate, w_up, w_down)


def plain_experts(normed, after, table, expert_weight, w_gate, w_up, w_down):
    row_count, top_count = expert_weight.shape
    expert_count = lax.axis_size("ep")
    capacity = table.shape[0] // expert_count
    width = normed.shape[1]
    repeated = jnp.repeat(normed, top_count, axis=0)
    sent = jnp.dot(table, repeated, preferred_element_type=jnp.float32).astype(jnp.bfloat16)
    sent = sent.reshape(expert_count, capacity, width)
    arrived = lax.all_to_all(sent, "ep", split_axis=0, concat_axis=0, tiled=True)
    flat = arrived.reshape(expert_count * capacity, width)
    piece = lax.all_gather(flat, "tp", axis=1, tiled=True)
    gate = jnp.dot(piece, w_gate[0], preferred_element_type=jnp.float32)
    upper = jnp.dot(piece, w_up[0], preferred_element_type=jnp.float32)
    hidden = (jax.nn.silu(gate) * upper).astype(jnp.bfloat16)
    partial_value = jnp.dot(hidden, w_down[0], preferred_element_type=jnp.float32)
    summed = lax.psum_scatter(
        partial_value.astype(jnp.bfloat16), "tp", scatter_dimension=1, tiled=True
    )
    results = summed.reshape(expert_count, capacity, width)
    returned = lax.all_to_all(results, "ep", split_axis=0, concat_axis=0, tiled=True)
    returned = returned.reshape(expert_count * capacity, width)
    picked = jnp.dot(table.T, returned, preferred_element_type=jnp.float32)
    picked = picked.reshape(row_count, top_count, width)
    weighted = jnp.sum(picked * expert_weight[..., None], axis=1)
    return (after.astype(jnp.float32) + weighted).astype(jnp.bfloat16)


def norm(values, gains):
    floats = values.astype(jnp.float32)
    scale = lax.rsqrt(jnp.mean(floats * floats, axis=1, keepdims=True) + 1e-06)
    return (floats * scale * gains).astype(jnp.bfloat16)


def power_of_two(count):
    return count & (count - 1) == 0


def body(
    tokens,
    gain_mix,
    w_in,
    decay_rate,
    frequency,
    log_step,
    input_real,
    input_imag,
    readout_real,
    readout_imaginary,
    passthrough_scale,
    state_real,
    state_imag,
    w_out,
    gain_ffn,
    expert_choice,
    expert_weight,
    w_gate,
    w_up,
    w_down,
):
    tp_count = lax.axis_size("tp")
    expert_count = lax.axis_size("ep")
    row_count, local_width = tokens.shape
    feature_start = lax.axis_index("tp") * local_width
    top_count = expert_choice.shape[1]
    capacity = 2 * row_count * top_count // expert_count
    table = slot_table(expert_choice, expert_count, capacity)
    all_tokens = lax.all_gather(tokens, "tp", axis=1, tiled=True)
    drive = jnp.dot(
        norm(all_tokens, gain_mix), w_in, preferred_element_type=jnp.float32
    ).astype(jnp.bfloat16)
    mixer, next_state_real, next_state_imaginary = state_step(
        drive,
        state_real,
        state_imag,
        decay_rate,
        frequency,
        log_step,
        input_real,
        input_imag,
        readout_real,
        readout_imaginary,
        passthrough_scale,
    )
    mixed = jnp.dot(
        lax.all_gather(mixer, "tp", axis=1, tiled=True), w_out, preferred_element_type=jnp.float32
    ).astype(jnp.bfloat16)
    after_all = (all_tokens.astype(jnp.float32) + mixed.astype(jnp.float32)).astype(jnp.bfloat16)
    normed_all = norm(after_all, gain_ffn)
    after = lax.dynamic_slice_in_dim(after_all, feature_start, local_width, 1)
    normed = lax.dynamic_slice_in_dim(normed_all, feature_start, local_width, 1)
    if (
        local_width % 128 == 0
        and w_gate.shape[2] % 128 == 0
        and capacity % 16 == 0
        and power_of_two(tp_count)
        and power_of_two(expert_count)
        and 2 < tp_count <= 8
        and 1 < expert_count <= 8
    ):
        pairs = table.reshape(expert_count * capacity, row_count, top_count)
        weights = jnp.sum(pairs.astype(jnp.float32) * expert_weight[None], axis=2).T
        high = lax.reduce_precision(weights, 8, 7)
        low = (weights - high).astype(jnp.bfloat16)
        layer_out = expert_call(
            normed,
            after,
            jnp.sum(pairs, axis=2),
            high.astype(jnp.bfloat16),
            low,
            w_gate,
            w_up,
            w_down,
            expert_count,
            tp_count,
        )
    else:
        layer_out = plain_experts(normed, after, table, expert_weight, w_gate, w_up, w_down)
    return (layer_out, next_state_real, next_state_imaginary)


def solution(mesh):
    return jax.shard_map(
        body,
        mesh=mesh,
        in_specs=(
            P("ep", "tp"),
            P(),
            P(None, "tp"),
            P("tp", None),
            P("tp", None),
            P("tp"),
            P("tp", None, None),
            P("tp", None, None),
            P("tp", None, None),
            P("tp", None, None),
            P("tp"),
            P("ep", "tp", None),
            P("ep", "tp", None),
            P(),
            P(),
            P("ep", None),
            P("ep", None),
            P("ep", None, "tp"),
            P("ep", None, "tp"),
            P("ep", "tp", None),
        ),
        out_specs=(P("ep", "tp"), P("ep", "tp", None), P("ep", "tp", None)),
        check_vma=False,
    )
```

```python
import functools

import jax
import jax.numpy as jnp
from jax import lax
from jax.experimental import pallas as pl
from jax.experimental.pallas import tpu as pltpu
from jax.sharding import PartitionSpec as P


def state_step(
    drive,
    real_state,
    imag_state,
    decay_rate,
    frequency,
    log_step,
    input_real,
    input_imag,
    readout_real,
    readout_imaginary,
    passthrough_scale,
):
    highest_precision = lax.Precision.HIGHEST
    count_of_groups, count_of_channels = (input_real.shape[0], input_real.shape[2])
    step = jnp.exp(log_step)[:, None]
    lam_real = -decay_rate
    magnitude = jnp.exp(lam_real * step)
    abar_real = magnitude * jnp.cos(frequency * step)
    abar_imag = magnitude * jnp.sin(frequency * step)
    denom = lam_real * lam_real + frequency * frequency
    numer = abar_real - 1.0
    factor_real = (numer * lam_real + abar_imag * frequency) / denom
    factor_imag = (abar_imag * lam_real - numer * frequency) / denom
    bbar_real = factor_real[..., None] * input_real - factor_imag[..., None] * input_imag
    bbar_imag = factor_real[..., None] * input_imag + factor_imag[..., None] * input_real
    float_values = drive.astype(jnp.float32).reshape(
        drive.shape[0], count_of_groups, count_of_channels
    )
    push_real = jnp.einsum("sgc,gpc->sgp", float_values, bbar_real, precision=highest_precision)
    push_imag = jnp.einsum("sgc,gpc->sgp", float_values, bbar_imag, precision=highest_precision)
    next_state_real = abar_real * real_state - abar_imag * imag_state + push_real
    next_state_imaginary = abar_real * imag_state + abar_imag * real_state + push_imag
    readout_matrix = (
        jnp.einsum("jdr,dyr->jdy", next_state_real, readout_real, precision=highest_precision)
        - jnp.einsum(
            "jdr,dyr->jdy", next_state_imaginary, readout_imaginary, precision=highest_precision
        )
        + passthrough_scale.reshape(count_of_groups, count_of_channels) * float_values
    )
    mixer = jax.nn.gelu(
        readout_matrix.reshape(drive.shape[0], count_of_groups * count_of_channels)
    ).astype(jnp.bfloat16)
    return (mixer, next_state_real, next_state_imaginary)


def slot_table(routes, expert_count, capacity):
    flat = routes.reshape(-1)
    onehot = (flat[:, None] == jnp.arange(expert_count, dtype=jnp.int32)[None, :]).astype(jnp.int32)
    before = jnp.cumsum(onehot, axis=0) - onehot
    slot = jnp.sum(before * onehot, axis=1)
    target = flat * capacity + slot
    return (
        target[None, :] == jnp.arange(expert_count * capacity, dtype=jnp.int32)[:, None]
    ).astype(jnp.bfloat16)


def flipped(index, mask, count):
    other = 0
    bit = 1
    while bit < count:
        digit = lax.rem(lax.div(index, bit), 2)
        other = other + bit * ((1 - digit) if mask & bit else digit)
        bit *= 2
    return other


def expert_kernel(
    ep_count,
    tp_count,
    mixer_ref,
    tokens_ref,
    gain_ref,
    choice_ref,
    weight_ref,
    out_w_hbm,
    gate_hbm,
    up_hbm,
    down_hbm,
    out_ref,
    mixers,
    out_w,
    after_buffer,
    gate_w,
    up_w,
    down_w,
    outgoing,
    arrived,
    gate_sum,
    up_sum,
    hidden,
    parts,
    parts_in,
    results,
    returned,
    mix_send,
    mix_recv,
    weight_sem,
    out_send,
    out_recv,
    near_send,
    near_recv,
    far_send,
    far_recv,
    part_send,
    part_recv,
    back_send,
    back_recv,
):
    me_ep, me_tp = lax.axis_index("ep"), lax.axis_index("tp")
    capacity, width = outgoing.shape[1], outgoing.shape[2]
    half = ep_count // 2
    peers = sorted(range(1, tp_count), key=lambda p: (bin(p).count("1"), p))
    near = [p for p in peers if bin(p).count("1") == 1]
    far = [p for p in peers if p not in near]
    tp_of = {p: flipped(me_tp, p, tp_count) for p in range(tp_count)}
    ep_of = {j: flipped(me_ep, j, ep_count) for j in range(ep_count)}

    def remote(src, dst, send, recv, **where):
        return pltpu.make_async_remote_copy(
            src_ref=src,
            dst_ref=dst,
            send_sem=send,
            recv_sem=recv,
            device_id=where,
            device_id_type=pl.DeviceIdType.MESH,
        )

    order = [0] + peers
    loads = {}
    channels = mixer_ref.shape[1]
    for p in order:
        rows = pl.ds(pl.multiple_of(tp_of[p] * channels, channels), channels)
        loads[3, p] = pltpu.make_async_copy(out_w_hbm.at[rows], out_w.at[p], weight_sem.at[3, p])
        loads[3, p].start()
    for p in order:
        rows = pl.ds(pl.multiple_of(tp_of[p] * width, width), width)
        loads[0, p] = pltpu.make_async_copy(gate_hbm.at[0, rows], gate_w.at[p], weight_sem.at[0, p])
        loads[1, p] = pltpu.make_async_copy(up_hbm.at[0, rows], up_w.at[p], weight_sem.at[1, p])
        loads[0, p].start()
        loads[1, p].start()
    down_order = far + near + [0]
    for p in down_order:
        columns = pl.ds(pl.multiple_of(tp_of[p] * width, width), width)
        loads[2, p] = pltpu.make_async_copy(
            down_hbm.at[0, :, columns], down_w.at[p], weight_sem.at[2, p]
        )
        loads[2, p].start()

    barrier = pltpu.get_barrier_semaphore()
    for p in peers:
        pl.semaphore_signal(
            barrier, inc=1, device_id={"tp": tp_of[p]}, device_id_type=pl.DeviceIdType.MESH
        )
    for j in range(1, ep_count):
        pl.semaphore_signal(
            barrier, inc=1, device_id={"ep": ep_of[j]}, device_id_type=pl.DeviceIdType.MESH
        )
    mixers[0] = mixer_ref[...]
    pl.semaphore_wait(barrier, len(peers) + ep_count - 1)
    mix_copies = {}
    for p in far + near:
        mix_copies[p] = remote(
            mixer_ref, mixers.at[p], mix_send.at[p], mix_recv.at[p], tp=tp_of[p]
        )
        mix_copies[p].start()

    row_count, top_count = choice_ref.shape
    choice, weight = choice_ref[...], weight_ref[...]
    spots = lax.broadcasted_iota(jnp.int32, (row_count, ep_count * capacity), 1)
    names = lax.broadcasted_iota(jnp.int32, (row_count, 128), 1)
    picks = [(choice[:, k : k + 1] == names).astype(jnp.float32) for k in range(top_count)]
    earlier = (
        lax.broadcasted_iota(jnp.int32, (row_count, row_count), 1)
        < lax.broadcasted_iota(jnp.int32, (row_count, row_count), 0)
    ).astype(jnp.float32)
    before = jnp.dot(
        earlier.astype(jnp.bfloat16),
        sum(picks).astype(jnp.bfloat16),
        preferred_element_type=jnp.float32,
    )
    table, weights = 0.0, 0.0
    for k in range(top_count):
        slot = jnp.sum(before * picks[k], axis=1, keepdims=True).astype(jnp.int32)
        hit = (choice[:, k : k + 1] * capacity + slot == spots).astype(jnp.float32)
        table = table + hit
        weights = weights + hit * weight[:, k : k + 1]
        before = before + picks[k]
    high = weights.astype(jnp.bfloat16)
    low = (weights - high.astype(jnp.float32)).astype(jnp.bfloat16)

    mixed = None
    for p in order:
        loads[3, p].wait()
        if p:
            mix_copies[p].wait_recv()
        term = jnp.dot(mixers[p], out_w[p], preferred_element_type=jnp.float32)
        mixed = term if mixed is None else mixed + term
    mixed = mixed.astype(jnp.bfloat16).astype(jnp.float32)
    after = (tokens_ref[...].astype(jnp.float32) + mixed).astype(jnp.bfloat16).astype(jnp.float32)
    scale = lax.rsqrt(jnp.mean(after * after, axis=1, keepdims=True) + 1e-06)
    after_buffer[...] = after
    own = pl.ds(pl.multiple_of(me_tp * width, width), width)
    normed = (after_buffer[:, own] * scale * gain_ref[:, own]).astype(jnp.bfloat16)
    sent = jnp.dot(table.T.astype(jnp.bfloat16), normed, preferred_element_type=jnp.float32)
    outgoing[...] = sent.astype(jnp.bfloat16).reshape(outgoing.shape)
    arrived[0, 0] = outgoing[me_ep]

    out_copies = {}
    for j in range(1, ep_count):
        out_copies[j] = remote(
            outgoing.at[ep_of[j]], arrived.at[0, j], out_send.at[j], out_recv.at[j], ep=ep_of[j]
        )
        out_copies[j].start()
    near_copies, far_copies = {}, {}
    for part in range(2):
        for j in range(part * half, part * half + half):
            if j:
                out_copies[j].wait_recv()
            for p in near:
                near_copies[p, j] = remote(
                    arrived.at[0, j],
                    arrived.at[p, j],
                    near_send.at[p, j],
                    near_recv.at[p, j],
                    tp=tp_of[p],
                )
                near_copies[p, j].start()
        for p in far:
            blocks = pl.ds(part * half, half)
            far_copies[p, part] = remote(
                arrived.at[0, blocks],
                arrived.at[p, blocks],
                far_send.at[p, part],
                far_recv.at[p, part],
                tp=tp_of[p],
            )
            far_copies[p, part].start()

    rows = ep_count * capacity
    hidden_width = hidden.shape[1]
    tile = next(t for t in (512, 256, 128) if hidden_width % t == 0)
    for place, p in enumerate(order):
        if p in near:
            for j in range(ep_count):
                near_copies[p, j].wait_recv()
        elif p:
            for part in range(2):
                far_copies[p, part].wait_recv()
        loads[0, p].wait()
        loads[1, p].wait()

        @pl.loop(0, hidden_width // tile)
        def _(n, place=place, p=p):
            columns = pl.ds(pl.multiple_of(n * tile, tile), tile)
            block = arrived[p].reshape(rows, width)
            gate = jnp.dot(block, gate_w[p, :, columns], preferred_element_type=jnp.float32)
            upper = jnp.dot(block, up_w[p, :, columns], preferred_element_type=jnp.float32)
            if place:
                gate = gate + gate_sum[:, columns]
                upper = upper + up_sum[:, columns]
            if place == len(order) - 1:
                hidden[:, columns] = (jax.nn.silu(gate) * upper).astype(jnp.bfloat16)
            else:
                gate_sum[:, columns] = gate
                up_sum[:, columns] = upper

    def part_copy(p, part):
        blocks = pl.ds((1 - part) * half * capacity, half * capacity)
        return remote(
            parts.at[p, blocks],
            parts_in.at[p, blocks],
            part_send.at[p, part],
            part_recv.at[p, part],
            tp=tp_of[p],
        )

    part_copies = {(p, part): part_copy(p, part) for p in peers for part in range(2)}
    cut = next(t for t in (256, 128) if width % t == 0)
    for p in down_order:
        loads[2, p].wait()

        @pl.loop(0, width // cut)
        def _(n, p=p):
            columns = pl.ds(pl.multiple_of(n * cut, cut), cut)
            parts[p, :, columns] = jnp.dot(
                hidden[...], down_w[p, :, columns], preferred_element_type=jnp.float32
            ).astype(jnp.bfloat16)

        if p:
            part_copies[p, 0].start()
        if p == down_order[-2]:
            for q in down_order[:-1]:
                part_copies[q, 1].start()

    back_copies = {}
    for part in range(2):
        blocks = pl.ds((1 - part) * half * capacity, half * capacity)
        total = None
        for p in range(tp_count):
            if p:
                part_copies[p, part].wait_recv()
                piece = parts_in[p, blocks].astype(jnp.float32)
            else:
                piece = parts[0, blocks].astype(jnp.float32)
            total = piece if total is None else total + piece
        first = (1 - part) * half
        results[pl.ds(first, half)] = total.astype(jnp.bfloat16).reshape(half, capacity, width)
        for j in reversed(range(first, first + half)):
            if j:
                back_copies[j] = remote(
                    results.at[j],
                    returned.at[me_ep],
                    back_send.at[j],
                    back_recv.at[j],
                    ep=ep_of[j],
                )
                back_copies[j].start()
    returned[me_ep] = results[0]
    for j in range(1, ep_count):
        remote(
            results.at[j], returned.at[ep_of[j]], back_send.at[j], back_recv.at[j], ep=ep_of[j]
        ).wait_recv()
    everything = returned[...].reshape(rows, width)
    weighted = jnp.dot(high, everything, preferred_element_type=jnp.float32)
    weighted = weighted + jnp.dot(low, everything, preferred_element_type=jnp.float32)
    out_ref[...] = (after_buffer[:, own] + weighted).astype(jnp.bfloat16)
    for copies in (mix_copies, out_copies, near_copies, far_copies, part_copies, back_copies):
        for copy in copies.values():
            copy.wait_send()


def gather_kernel(
    tp_count,
    tokens_ref,
    gain_ref,
    weight_hbm,
    all_ref,
    drive_ref,
    pieces,
    weight,
    load_sem,
    send_sem,
    recv_sem,
):
    me_tp = lax.axis_index("tp")
    width = tokens_ref.shape[1]
    tp_of = {p: flipped(me_tp, p, tp_count) for p in range(tp_count)}
    order = sorted(range(tp_count), key=lambda p: (bin(p).count("1"), p))
    loads, copies = {}, {}
    for p in order:
        rows = pl.ds(pl.multiple_of(tp_of[p] * width, width), width)
        loads[p] = pltpu.make_async_copy(weight_hbm.at[rows], weight.at[p], load_sem.at[p])
        loads[p].start()
    barrier = pltpu.get_barrier_semaphore()
    for p in order[1:]:
        pl.semaphore_signal(
            barrier, inc=1, device_id={"tp": tp_of[p]}, device_id_type=pl.DeviceIdType.MESH
        )
    pl.semaphore_wait(barrier, tp_count - 1)
    for p in order[1:]:
        copies[p] = pltpu.make_async_remote_copy(
            src_ref=tokens_ref,
            dst_ref=pieces.at[p],
            send_sem=send_sem.at[p],
            recv_sem=recv_sem.at[p],
            device_id={"tp": tp_of[p]},
            device_id_type=pl.DeviceIdType.MESH,
        )
        copies[p].start()
    pieces[0] = tokens_ref[...]
    squares = 0.0
    for p in order:
        if p:
            copies[p].wait_recv()
        piece = pieces[p]
        all_ref[:, pl.ds(pl.multiple_of(tp_of[p] * width, width), width)] = piece
        floats = piece.astype(jnp.float32)
        squares = squares + jnp.sum(floats * floats, axis=1, keepdims=True)
    scale = lax.rsqrt(squares / (width * tp_count) + 1e-06)
    drive = None
    for p in order:
        normed = (pieces[p].astype(jnp.float32) * scale * gain_ref[tp_of[p]]).astype(jnp.bfloat16)
        loads[p].wait()
        term = jnp.dot(normed, weight[p], preferred_element_type=jnp.float32)
        drive = term if drive is None else drive + term
    drive_ref[...] = drive.astype(jnp.bfloat16)
    for p in order[1:]:
        copies[p].wait_send()


def gather_call(tokens, gain, w_in, tp_count):
    row_count, width = tokens.shape
    channels = w_in.shape[1]
    dma = pltpu.SemaphoreType.DMA((tp_count,))
    vmem = pl.BlockSpec(memory_space=pltpu.VMEM)
    return pl.pallas_call(
        functools.partial(gather_kernel, tp_count),
        out_shape=(
            jax.ShapeDtypeStruct((row_count, width * tp_count), jnp.bfloat16),
            jax.ShapeDtypeStruct((row_count, channels), jnp.bfloat16),
        ),
        in_specs=[vmem, vmem, pl.BlockSpec(memory_space=pl.ANY)],
        out_specs=(vmem, vmem),
        scratch_shapes=[
            pltpu.VMEM((tp_count, row_count, width), jnp.bfloat16),
            pltpu.VMEM((tp_count, width, channels), jnp.bfloat16),
            dma,
            dma,
            dma,
        ],
        compiler_params=pltpu.CompilerParams(collective_id=1, has_side_effects=True),
    )(tokens, gain.reshape(tp_count, 1, width), w_in)


def expert_call(
    mixer, tokens, gain, choice, weight, w_out, w_gate, w_up, w_down, capacity, ep_count, tp_count
):
    row_count, full_width = tokens.shape
    channels = mixer.shape[1]
    width = full_width // tp_count
    slots = ep_count * capacity
    hidden_width = w_gate.shape[2]
    bf16, f32 = jnp.bfloat16, jnp.float32
    dma = pltpu.SemaphoreType.DMA
    vmem = pl.BlockSpec(memory_space=pltpu.VMEM)
    hbm = pl.BlockSpec(memory_space=pl.ANY)
    return pl.pallas_call(
        functools.partial(expert_kernel, ep_count, tp_count),
        out_shape=jax.ShapeDtypeStruct((row_count, width), bf16),
        in_specs=[vmem] * 5 + [hbm] * 4,
        out_specs=vmem,
        scratch_shapes=[
            pltpu.VMEM((tp_count, row_count, channels), bf16),
            pltpu.VMEM((tp_count, channels, full_width), bf16),
            pltpu.VMEM((row_count, full_width), f32),
            pltpu.VMEM((tp_count, width, hidden_width), bf16),
            pltpu.VMEM((tp_count, width, hidden_width), bf16),
            pltpu.VMEM((tp_count, hidden_width, width), bf16),
            pltpu.VMEM((ep_count, capacity, width), bf16),
            pltpu.VMEM((tp_count, ep_count, capacity, width), bf16),
            pltpu.VMEM((slots, hidden_width), f32),
            pltpu.VMEM((slots, hidden_width), f32),
            pltpu.VMEM((slots, hidden_width), bf16),
            pltpu.VMEM((tp_count, slots, width), bf16),
            pltpu.VMEM((tp_count, slots, width), bf16),
            pltpu.VMEM((ep_count, capacity, width), bf16),
            pltpu.VMEM((ep_count, capacity, width), bf16),
            dma((tp_count,)),
            dma((tp_count,)),
            dma((4, tp_count)),
            dma((ep_count,)),
            dma((ep_count,)),
            dma((tp_count, ep_count)),
            dma((tp_count, ep_count)),
            dma((tp_count, 2)),
            dma((tp_count, 2)),
            dma((tp_count, 2)),
            dma((tp_count, 2)),
            dma((ep_count,)),
            dma((ep_count,)),
        ],
        compiler_params=pltpu.CompilerParams(
            collective_id=0, has_side_effects=True, vmem_limit_bytes=60 * 1024 * 1024
        ),
    )(mixer, tokens, gain.reshape(1, full_width), choice, weight, w_out, w_gate, w_up, w_down)


def plain_experts(normed, after, table, expert_weight, w_gate, w_up, w_down):
    row_count, top_count = expert_weight.shape
    expert_count = lax.axis_size("ep")
    capacity = table.shape[0] // expert_count
    width = normed.shape[1]
    repeated = jnp.repeat(normed, top_count, axis=0)
    sent = jnp.dot(table, repeated, preferred_element_type=jnp.float32).astype(jnp.bfloat16)
    sent = sent.reshape(expert_count, capacity, width)
    arrived = lax.all_to_all(sent, "ep", split_axis=0, concat_axis=0, tiled=True)
    flat = arrived.reshape(expert_count * capacity, width)
    piece = lax.all_gather(flat, "tp", axis=1, tiled=True)
    gate = jnp.dot(piece, w_gate[0], preferred_element_type=jnp.float32)
    upper = jnp.dot(piece, w_up[0], preferred_element_type=jnp.float32)
    hidden = (jax.nn.silu(gate) * upper).astype(jnp.bfloat16)
    partial_value = jnp.dot(hidden, w_down[0], preferred_element_type=jnp.float32)
    summed = lax.psum_scatter(
        partial_value.astype(jnp.bfloat16), "tp", scatter_dimension=1, tiled=True
    )
    results = summed.reshape(expert_count, capacity, width)
    returned = lax.all_to_all(results, "ep", split_axis=0, concat_axis=0, tiled=True)
    returned = returned.reshape(expert_count * capacity, width)
    picked = jnp.dot(table.T, returned, preferred_element_type=jnp.float32)
    picked = picked.reshape(row_count, top_count, width)
    weighted = jnp.sum(picked * expert_weight[..., None], axis=1)
    return (after.astype(jnp.float32) + weighted).astype(jnp.bfloat16)


def norm(values, gains):
    floats = values.astype(jnp.float32)
    scale = lax.rsqrt(jnp.mean(floats * floats, axis=1, keepdims=True) + 1e-06)
    return (floats * scale * gains).astype(jnp.bfloat16)


def power_of_two(count):
    return count & (count - 1) == 0


def body(
    tokens,
    gain_mix,
    w_in,
    decay_rate,
    frequency,
    log_step,
    input_real,
    input_imag,
    readout_real,
    readout_imaginary,
    passthrough_scale,
    state_real,
    state_imag,
    w_out,
    gain_ffn,
    expert_choice,
    expert_weight,
    w_gate,
    w_up,
    w_down,
):
    tp_count = lax.axis_size("tp")
    expert_count = lax.axis_size("ep")
    row_count, local_width = tokens.shape
    feature_start = lax.axis_index("tp") * local_width
    top_count = expert_choice.shape[1]
    capacity = 2 * row_count * top_count // expert_count
    fused = (
        local_width % 128 == 0
        and w_gate.shape[2] % 128 == 0
        and capacity % 16 == 0
        and power_of_two(tp_count)
        and power_of_two(expert_count)
        and 2 < tp_count <= 8
        and 1 < expert_count <= 8
        and w_in.shape[1] % 128 == 0
        and row_count % 16 == 0
    )
    if fused:
        all_tokens, drive = gather_call(tokens, gain_mix, w_in, tp_count)
    else:
        all_tokens = lax.all_gather(tokens, "tp", axis=1, tiled=True)
        drive = jnp.dot(
            norm(all_tokens, gain_mix), w_in, preferred_element_type=jnp.float32
        ).astype(jnp.bfloat16)
    mixer, next_state_real, next_state_imaginary = state_step(
        drive,
        state_real,
        state_imag,
        decay_rate,
        frequency,
        log_step,
        input_real,
        input_imag,
        readout_real,
        readout_imaginary,
        passthrough_scale,
    )
    if fused:
        layer_out = expert_call(
            mixer,
            all_tokens,
            gain_ffn,
            expert_choice,
            expert_weight,
            w_out,
            w_gate,
            w_up,
            w_down,
            capacity,
            expert_count,
            tp_count,
        )
        return (layer_out, next_state_real, next_state_imaginary)
    table = slot_table(expert_choice, expert_count, capacity)
    mixed = jnp.dot(
        lax.all_gather(mixer, "tp", axis=1, tiled=True), w_out, preferred_element_type=jnp.float32
    ).astype(jnp.bfloat16)
    after_all = (all_tokens.astype(jnp.float32) + mixed.astype(jnp.float32)).astype(jnp.bfloat16)
    normed_all = norm(after_all, gain_ffn)
    after = lax.dynamic_slice_in_dim(after_all, feature_start, local_width, 1)
    normed = lax.dynamic_slice_in_dim(normed_all, feature_start, local_width, 1)
    layer_out = plain_experts(normed, after, table, expert_weight, w_gate, w_up, w_down)
    return (layer_out, next_state_real, next_state_imaginary)


def solution(mesh):
    return jax.shard_map(
        body,
        mesh=mesh,
        in_specs=(
            P("ep", "tp"),
            P(),
            P(None, "tp"),
            P("tp", None),
            P("tp", None),
            P("tp"),
            P("tp", None, None),
            P("tp", None, None),
            P("tp", None, None),
            P("tp", None, None),
            P("tp"),
            P("ep", "tp", None),
            P("ep", "tp", None),
            P(),
            P(),
            P("ep", None),
            P("ep", None),
            P("ep", None, "tp"),
            P("ep", None, "tp"),
            P("ep", "tp", None),
        ),
        out_specs=(P("ep", "tp"), P("ep", "tp", None), P("ep", "tp", None)),
        check_vma=False,
    )
```
